512 devices in a mesh: grp: 2 (over y), kv: 32 (over z), tp: 8 (over x, core).
Axes of the slice: x: 4, y: 2, z: 32, core: 2. Of those that a mesh axis runs over, the one named last changes fastest.
The devices are a block of a 4x8x32 slice.
Arguments:
- tokens: bfloat16 [256, 4096], P('grp', ('kv', 'tp')), parts along dimension 0, may hold values from -50 to 50
- mix_gain: bfloat16 [4096], P('kv'), may hold values from 0.099609375 to 1.8984375
- w_query: bfloat16 [4096, 2048], P('kv', 'tp'), may hold values from -0.09375 to 0.09375
- w_forget: bfloat16 [4096, 2048], P('kv', 'tp'), may hold values from -0.09375 to 0.09375
- w_input: bfloat16 [4096, 2048], P('kv', 'tp'), may hold values from -0.09375 to 0.09375
- w_outgate: bfloat16 [4096, 2048], P('kv', 'tp'), may hold values from -0.09375 to 0.09375
- lower_bound: float32 [2048], P('tp'), may hold values from 0.05 to 0.9
- state: float32 [256, 16, 128, 128], P(('grp', 'kv'), 'tp'), parts along dimension 0, may hold values from -4 to 4
- head_gain: bfloat16 [128], replicated, may hold values from 0.099609375 to 1.8984375
- w_mixout: bfloat16 [2048, 4096], P('tp', 'kv'), may hold values from -0.125 to 0.125
- ffn_gain: bfloat16 [4096], P('kv'), may hold values from 0.099609375 to 1.8984375
- w_gate: bfloat16 [4096, 11264], P('kv', 'tp'), may hold values from -0.09375 to 0.09375
- w_up: bfloat16 [4096, 11264], P('kv', 'tp'), may hold values from -0.09375 to 0.09375
- w_down: bfloat16 [11264, 4096], P('tp', 'kv'), may hold values from -0.0546875 to 0.0546875
Outputs:
- mixed: bfloat16 [256, 4096], P('grp', ('kv', 'tp')), parts along dimension 0
- new_state: float32 [256, 16, 128, 128], P(('grp', 'kv'), 'tp'), parts along dimension 0
The draws below stay inside these ranges and needn't reach their ends.
There are 2 independent parts, one for each index of `grp`. The reference program is written for one: setup_inputs(seed, part) draws one part's arguments, and reference() takes and returns one part's arrays. A program takes and returns all parts, laid end to end along the dimension named above; an argument that names none is the same for every part. Nothing has to cross between parts.
All inputs are finite; a program needn't handle non-finite values.
Results may differ from the reference program's by a relative error of at most 0.01.
Values may be sent and summed in bfloat16 or wider, within the bound.
No kernel may reach another device: no remote copies, remote signals or barrier semaphores. Data moves between devices by JAX's collectives and lax.ppermute only.
A program may use at most 64 MiB of HBM per device.

```python
import jax
import jax.numpy as jnp
from jax import lax

D = 4096
HEADS = 16
HEAD_DIM = 128
FF = 11264
BATCH = 128
KEY_WIDTH = 2048


def draw_tokens(key, part):
    key_base = jax.random.fold_in(key, 11)
    key_cols = jax.random.fold_in(key, 12)
    block_scale = jnp.exp(jax.random.uniform(key_cols, (D // 16,), jnp.float32, -1.1, 1.1))
    column_scale = jnp.repeat(block_scale, 16)[None, :]
    base = jnp.clip(jax.random.normal(key_base, (BATCH, D), jnp.float32), -4.0, 4.0)
    return (base * column_scale).astype(jnp.bfloat16)


def shard_levels(rng, shape, cuts, low, largest):
    def one(position, blocks):
        draws = jax.random.uniform(jax.random.fold_in(jax.random.fold_in(rng, 6), position), (blocks,), jnp.float32, low / len(cuts), largest / len(cuts))
        return jnp.repeat(jnp.exp(draws), shape[position] // blocks).reshape((-1,) + (1,) * (len(shape) - position - 1))

    loudness = one(*cuts[0])
    for cut in cuts[1:]:
        loudness = loudness * one(*cut)
    return loudness


def noise(key, dims, width, most, pieces=(), kind=jnp.bfloat16):
    entries = jax.random.normal(key, dims, jnp.float32) * width
    if len(pieces) > 0:
        entries = shard_levels(key, dims, pieces, -0.22, 0.18) * entries
    return jnp.clip(entries, min=-most, max=most).astype(kind)


def setup_inputs(seed: int = 0, part: int = 0) -> dict:
    arg_keys = jax.random.split(jax.random.key(seed), 15)
    part_splits = jax.random.split(jax.random.fold_in(arg_keys[14], part), 15)
    return {
        "tokens": draw_tokens(jax.random.fold_in(jax.random.fold_in(arg_keys[14], part), 71), part),
        "mix_gain": jnp.clip(1.0 + 0.18 * jax.random.normal(arg_keys[1], (D,), jnp.float32), 0.099609375, 1.8984375).astype(jnp.bfloat16),
        "w_query": noise(arg_keys[2], (D, KEY_WIDTH), D ** -0.5, 0.09375, ((0, 32), (1, 8))),
        "w_forget": noise(arg_keys[3], (D, KEY_WIDTH), D ** -0.5, 0.09375, ((0, 32), (1, 8))),
        "w_input": noise(arg_keys[4], (D, KEY_WIDTH), D ** -0.5, 0.09375, ((0, 32), (1, 8))),
        "w_outgate": noise(arg_keys[5], (D, KEY_WIDTH), D ** -0.5, 0.09375, ((0, 32), (1, 8))),
        "lower_bound": jnp.clip(0.05 + 0.84999998 * jax.random.uniform(arg_keys[6], (KEY_WIDTH,), jnp.float32) ** shard_levels(arg_keys[6], (KEY_WIDTH,), ((0, 8),), -0.2, 0.2), 0.05, 0.9),
        "state": noise(part_splits[7], (BATCH, HEADS, HEAD_DIM, HEAD_DIM), 0.5, 4.0, ((0, 32), (1, 8)), jnp.float32),
        "head_gain": jnp.clip(1.0 + 0.18 * jax.random.normal(arg_keys[8], (HEAD_DIM,), jnp.float32), 0.099609375, 1.8984375).astype(jnp.bfloat16),
        "w_mixout": noise(arg_keys[9], (KEY_WIDTH, D), KEY_WIDTH ** -0.5, 0.125, ((0, 8), (1, 32))),
        "ffn_gain": jnp.clip(1.0 + 0.18 * jax.random.normal(arg_keys[10], (D,), jnp.float32), 0.099609375, 1.8984375).astype(jnp.bfloat16),
        "w_gate": noise(arg_keys[11], (D, FF), D ** -0.5, 0.09375, ((0, 32), (1, 8))),
        "w_up": noise(arg_keys[12], (D, FF), D ** -0.5, 0.09375, ((0, 32), (1, 8))),
        "w_down": noise(arg_keys[13], (FF, D), FF ** -0.5, 0.0546875, ((0, 8), (1, 32))),
    }


eps = 0.1

def reference(tokens, mix_gain, w_query, w_forget, w_input, w_outgate, lower_bound, state, head_gain, w_mixout, ffn_gain, w_gate, w_up, w_down):
    batch = tokens.shape[0]
    tokens_f = tokens.astype(jnp.float32)
    normed = (tokens_f * mix_gain.astype(jnp.float32)).astype(jnp.bfloat16)
    inv_rms = lax.rsqrt(lax.optimization_barrier(jnp.mean(tokens_f * tokens_f, axis=1, keepdims=True)) + eps)

    def heads_of(weight):
        product = jnp.dot(normed, weight, preferred_element_type=jnp.float32) * inv_rms
        return product.reshape(batch, HEADS, HEAD_DIM)
    query_act = jax.nn.silu(heads_of(w_query))
    forget_raw = heads_of(w_forget)
    values_in = heads_of(w_input)
    gate_raw = heads_of(w_outgate)
    bounds = lower_bound.reshape(HEADS, HEAD_DIM)
    forget = bounds + (1.0 - bounds) * jax.nn.sigmoid(forget_raw)
    key_in = (1.0 - bounds) * jax.nn.sigmoid(-forget_raw)
    new_state = forget[..., None] * state + key_in[..., None] * values_in[:, :, None, :]
    readout = lax.optimization_barrier(jnp.sum(query_act[..., None] * new_state, axis=2))
    head_rms = lax.rsqrt(lax.optimization_barrier(jnp.mean(readout * readout, axis=-1, keepdims=True)) + eps)
    gated_out = readout * head_rms * head_gain.astype(jnp.float32) * jax.nn.silu(gate_raw)
    gated_out = gated_out.reshape(batch, HEADS * HEAD_DIM).astype(jnp.bfloat16)
    mix_sum = jnp.dot(gated_out, w_mixout, preferred_element_type=jnp.float32)
    resid = (tokens_f + mix_sum).astype(jnp.bfloat16)
    resid_f = resid.astype(jnp.float32)
    normed_ffn = (resid_f * ffn_gain.astype(jnp.float32)).astype(jnp.bfloat16)
    inv_rms_ffn = lax.rsqrt(lax.optimization_barrier(jnp.mean(resid_f * resid_f, axis=1, keepdims=True)) + eps)
    gate_sum = jnp.dot(normed_ffn, w_gate, preferred_element_type=jnp.float32) * inv_rms_ffn
    up_sum = jnp.dot(normed_ffn, w_up, preferred_element_type=jnp.float32) * inv_rms_ffn
    hidden = (jax.nn.silu(gate_sum) * up_sum).astype(jnp.bfloat16)
    down_sum = jnp.dot(hidden, w_down, preferred_element_type=jnp.float32)
    mixed = (resid_f + down_sum).astype(jnp.bfloat16)
    return (mixed, new_state)
```

```python
import jax
import jax.numpy as jnp
from jax import lax
from jax.sharding import PartitionSpec as P

D = 4096
NEAR = 4

eps = 0.1
bf16, f32 = jnp.bfloat16, jnp.float32


def spread(parts, axis, groups=None):
    return lax.all_to_all(parts, axis, 0, 0, axis_index_groups=groups, tiled=True)


def share(array, axis, size, groups=None):
    return spread(jnp.broadcast_to(array[None], (size, *array.shape)), axis, groups)


def summed(parts):
    return jnp.sum(parts.astype(f32), axis=0)


def dot_t(left, right, contract):
    return lax.dot_general(left, right, (contract, ((), ())), preferred_element_type=f32)


def pick(stack, index):
    return lax.dynamic_index_in_dim(stack, index, 0, keepdims=False)


def exchanged(stack, place, groups):
    got = [pick(stack, place)]
    for k in range(1, NEAR):
        pairs = [(g[i], g[i ^ k]) for g in groups for i in range(NEAR)]
        got.append(lax.ppermute(pick(stack, place ^ k), "kv", pairs))
    got = jnp.stack(got)
    return jnp.stack([pick(got, j ^ place) for j in range(NEAR)])


def body(
    tokens,
    mix_gain,
    w_query,
    w_forget,
    w_input,
    w_outgate,
    lower_bound,
    state,
    head_gain,
    w_mixout,
    ffn_gain,
    w_gate,
    w_up,
    w_down,
):
    rows_here, heads_here, head_size = state.shape[:3]
    kv, tp = lax.axis_size("kv"), lax.axis_size("tp")
    batch, own_width = tokens.shape
    far = kv // NEAR
    near_groups = [[NEAR * a + b for b in range(NEAR)] for a in range(far)]
    far_groups = [[NEAR * a + b for a in range(far)] for b in range(NEAR)]
    block_groups = [
        [(NEAR * a + b) * tp + t for b in range(NEAR) for t in range(tp)] for a in range(far)
    ]
    place = lax.axis_index("kv") % NEAR

    units = w_gate.shape[1] // NEAR
    width = -(-(2 * units + 1) // 128) * 128
    pad = jnp.zeros((w_gate.shape[0], width - 2 * units - 1), bf16)
    cut = lambda w, j: w[:, j * units : (j + 1) * units]
    pieces = jnp.stack(
        [
            jnp.concatenate([cut(w_gate, j), cut(w_up, j), ffn_gain[:, None], pad], axis=1)
            for j in range(NEAR)
        ]
    )
    w_gate_up = exchanged(pieces, place, near_groups).reshape(-1, width)
    w_out = exchanged(w_down.reshape(NEAR, units, -1), place, near_groups)

    block = share(tokens.T, "tp", tp).reshape(-1, batch)
    block_f = block.astype(f32)
    normed = (block_f * mix_gain.astype(f32)[:, None]).astype(bf16)
    squares = jnp.sum(block_f * block_f, axis=0)
    weights = (w_query, w_forget, w_input, w_outgate)
    terms = [dot_t(normed, w, ((0,), (0,))).astype(bf16) for w in weights]
    side = jnp.broadcast_to(squares.astype(bf16)[:, None], (batch, 128))
    terms = jnp.concatenate(terms + [side], axis=1)
    terms = terms.reshape(far, NEAR, rows_here, -1).transpose(1, 0, 2, 3)
    terms = summed(spread(terms, "kv", near_groups)).astype(bf16)
    sums = summed(spread(terms, "kv", far_groups))
    key_width = heads_here * head_size
    inv_rms = lax.rsqrt(sums[:, 4 * key_width : 4 * key_width + 1] / D + eps)
    raw = [
        (sums[:, i * key_width : (i + 1) * key_width] * inv_rms).reshape(
            rows_here, heads_here, head_size
        )
        for i in range(4)
    ]

    query_act = jax.nn.silu(raw[0])
    bounds = lower_bound.reshape(heads_here, head_size)
    forget = bounds + (1.0 - bounds) * jax.nn.sigmoid(raw[1])
    key_in = (1.0 - bounds) * jax.nn.sigmoid(-raw[1])
    new_state = forget[..., None] * state + key_in[..., None] * raw[2][:, :, None, :]
    readout = jnp.sum(query_act[..., None] * new_state, axis=2)
    head_rms = lax.rsqrt(jnp.mean(readout * readout, axis=-1, keepdims=True) + eps)
    gated = readout * head_rms * head_gain.astype(f32) * jax.nn.silu(raw[3])
    gated = gated.reshape(rows_here, key_width).astype(bf16)

    gated_all = share(gated, "kv", kv).reshape(batch, key_width)
    mix = dot_t(w_mixout, gated_all, ((0,), (1,))).astype(bf16)
    resid = (block_f + summed(share(mix, "tp", tp))).astype(bf16)
    resid_own = lax.dynamic_slice_in_dim(resid, lax.axis_index("tp") * own_width, own_width, 0)

    resid_f = share(resid, "kv", NEAR, near_groups).reshape(-1, batch).astype(f32)
    gain = w_gate_up[:, 2 * units : 2 * units + 1].astype(f32)
    normed_ffn = (resid_f * gain).astype(bf16)
    squares_ffn = jnp.sum(resid_f * resid_f, axis=0)
    terms = dot_t(normed_ffn, w_gate_up, ((0,), (0,)))
    column = lax.broadcasted_iota(jnp.int32, terms.shape, 1)
    terms = jnp.where(column == 2 * units, squares_ffn[:, None], terms).astype(bf16)
    sums = summed(spread(terms.reshape(far, -1, width), "kv", far_groups))
    inv_rms = lax.rsqrt(sums[:, 2 * units : 2 * units + 1] / D + eps)
    gate_sum, up_sum = sums[:, :units] * inv_rms, sums[:, units : 2 * units] * inv_rms
    hidden = (jax.nn.silu(gate_sum) * up_sum).astype(bf16)
    hidden_all = share(hidden, "kv", far, far_groups).reshape(batch, units)
    down = dot_t(w_out, hidden_all, ((1,), (1,))).astype(bf16)
    down = summed(spread(down.reshape(NEAR * tp, own_width, batch), ("kv", "tp"), block_groups))
    mixed = (resid_own.astype(f32) + down).astype(bf16).T
    return (mixed, new_state)


def solution(mesh):
    return jax.shard_map(
        body,
        mesh=mesh,
        in_specs=(
            P("grp", ("kv", "tp")),
            P("kv"),
            P("kv", "tp"),
            P("kv", "tp"),
            P("kv", "tp"),
            P("kv", "tp"),
            P("tp"),
            P(("grp", "kv"), "tp", None, None),
            P(),
            P("tp", "kv"),
            P("kv"),
            P("kv", "tp"),
            P("kv", "tp"),
            P("tp", "kv"),
        ),
        out_specs=(P("grp", ("kv", "tp")), P(("grp", "kv"), "tp", None, None)),
        check_vma=False,
    )
```

```python
import jax
import jax.numpy as jnp
from jax import lax
from jax.sharding import PartitionSpec as P


D = 4096
NEAR = 4

eps = 0.1
bf16, f32 = jnp.bfloat16, jnp.float32


def spread(parts, axis, groups=None):
    return lax.all_to_all(parts, axis, 0, 0, axis_index_groups=groups, tiled=True)


def share(array, axis, size, groups=None):
    return spread(jnp.broadcast_to(array[None], (size, *array.shape)), axis, groups)


def summed(parts):
    return jnp.sum(parts.astype(f32), axis=0)


def dot_t(left, right, contract):
    return lax.dot_general(left, right, (contract, ((), ())), preferred_element_type=f32)


def pick(stack, index):
    return lax.dynamic_index_in_dim(stack, index, 0, keepdims=False)


def exchanged(stack, place, groups):
    got = [pick(stack, place)]
    for k in range(1, NEAR):
        pairs = [(g[i], g[i ^ k]) for g in groups for i in range(NEAR)]
        got.append(lax.ppermute(pick(stack, place ^ k), "kv", pairs))
    got = jnp.stack(got)
    return jnp.stack([pick(got, j ^ place) for j in range(NEAR)])


def step(
    tokens,
    mix_gain,
    w_query,
    w_forget,
    w_input,
    w_outgate,
    lower_bound,
    state,
    head_gain,
    w_mixout,
    ffn_gain,
    w_gate,
    w_up,
    w_down,
):
    rows_here, heads_here, head_size = state.shape[:3]
    kv, tp = lax.axis_size("kv"), lax.axis_size("tp")
    batch, own_width = tokens.shape
    far = kv // NEAR
    near_groups = [[NEAR * a + b for b in range(NEAR)] for a in range(far)]
    far_groups = [[NEAR * a + b for a in range(far)] for b in range(NEAR)]
    block_groups = [
        [(NEAR * a + b) * tp + t for b in range(NEAR) for t in range(tp)] for a in range(far)
    ]
    place = lax.axis_index("kv") % NEAR

    units = w_gate.shape[1] // NEAR
    width = -(-(2 * units + 1) // 128) * 128
    pad = jnp.zeros((w_gate.shape[0], width - 2 * units - 1), bf16)
    cut = lambda w, j: w[:, j * units : (j + 1) * units]
    pieces = jnp.stack(
        [
            jnp.concatenate([cut(w_gate, j), cut(w_up, j), ffn_gain[:, None], pad], axis=1)
            for j in range(NEAR)
        ]
    )
    w_gate_up = exchanged(pieces, place, near_groups).reshape(-1, width)
    w_out = exchanged(w_down.reshape(NEAR, units, -1), place, near_groups)

    block = share(tokens.T, "tp", tp).reshape(-1, batch)
    block_f = block.astype(f32)
    normed = (block_f * mix_gain.astype(f32)[:, None]).astype(bf16)
    squares = jnp.sum(block_f * block_f, axis=0)
    weights = jnp.concatenate([w_query, w_forget, w_input, w_outgate], axis=1)
    terms = dot_t(normed, lax.optimization_barrier(weights), ((0,), (0,))).astype(bf16)
    side = jnp.broadcast_to(squares.astype(bf16)[:, None], (batch, 128))
    terms = jnp.concatenate([terms, side], axis=1)
    terms = terms.reshape(far, NEAR, rows_here, -1).transpose(1, 0, 2, 3)
    terms = summed(spread(terms, "kv", near_groups)).astype(bf16)
    sums = spread(terms, "kv", far_groups)
    sums = summed(sums)
    key_width = heads_here * head_size
    inv_rms = lax.rsqrt(sums[:, 4 * key_width : 4 * key_width + 1] / D + eps)
    raw = [
        (sums[:, i * key_width : (i + 1) * key_width] * inv_rms).reshape(
            rows_here, heads_here, head_size
        )
        for i in range(4)
    ]

    query_act = jax.nn.silu(raw[0])
    bounds = lower_bound.reshape(heads_here, head_size)
    forget = bounds + (1.0 - bounds) * jax.nn.sigmoid(raw[1])
    key_in = (1.0 - bounds) * jax.nn.sigmoid(-raw[1])
    new_state = forget[..., None] * state + key_in[..., None] * raw[2][:, :, None, :]
    readout = jnp.sum(query_act[..., None] * new_state, axis=2)
    head_rms = lax.rsqrt(jnp.mean(readout * readout, axis=-1, keepdims=True) + eps)
    gated = readout * head_rms * head_gain.astype(f32) * jax.nn.silu(raw[3])
    gated = gated.reshape(rows_here, key_width).astype(bf16)

    gated_all = share(gated, "kv", kv).reshape(batch, key_width)
    mix = dot_t(w_mixout, gated_all, ((0,), (1,))).astype(bf16)
    resid = (block_f + summed(share(mix, "tp", tp))).astype(bf16)
    resid_own = lax.dynamic_slice_in_dim(resid, lax.axis_index("tp") * own_width, own_width, 0)

    resid_f = share(resid, "kv", NEAR, near_groups).reshape(-1, batch).astype(f32)
    gain = w_gate_up[:, 2 * units : 2 * units + 1].astype(f32)
    normed_ffn = (resid_f * gain).astype(bf16)
    squares_ffn = jnp.sum(resid_f * resid_f, axis=0)
    terms = dot_t(normed_ffn, w_gate_up, ((0,), (0,)))
    column = lax.broadcasted_iota(jnp.int32, terms.shape, 1)
    terms = jnp.where(column == 2 * units, squares_ffn[:, None], terms).astype(bf16)
    sums = summed(spread(terms.reshape(far, -1, width), "kv", far_groups))
    inv_rms = lax.rsqrt(sums[:, 2 * units : 2 * units + 1] / D + eps)
    gate_sum, up_sum = sums[:, :units] * inv_rms, sums[:, units : 2 * units] * inv_rms
    hidden = (jax.nn.silu(gate_sum) * up_sum).astype(bf16)
    hidden_all = share(hidden, "kv", far, far_groups).reshape(batch, units)
    down = dot_t(w_out, hidden_all, ((1,), (1,))).astype(bf16)
    down = summed(spread(down.reshape(NEAR * tp, own_width, batch), ("kv", "tp"), block_groups))
    mixed = (resid_own.astype(f32) + down).astype(bf16).T
    return (mixed, new_state)


def solution(mesh):
    return jax.shard_map(
        step,
        mesh=mesh,
        in_specs=(
            P("grp", ("kv", "tp")),
            P("kv"),
            P("kv", "tp"),
            P("kv", "tp"),
            P("kv", "tp"),
            P("kv", "tp"),
            P("tp"),
            P(("grp", "kv"), "tp", None, None),
            P(),
            P("tp", "kv"),
            P("kv"),
            P("kv", "tp"),
            P("kv", "tp"),
            P("tp", "kv"),
        ),
        out_specs=(P("grp", ("kv", "tp")), P(("grp", "kv"), "tp", None, None)),
        check_vma=False,
    )
```

```python
import jax
import jax.numpy as jnp
from jax import lax
from jax.sharding import PartitionSpec as P


D = 4096
NEAR = 4

eps = 0.1
bf16, f32 = jnp.bfloat16, jnp.float32


def spread(parts, axis, groups=None):
    return lax.all_to_all(parts, axis, 0, 0, axis_index_groups=groups, tiled=True)


def share(array, axis, size, groups=None):
    return spread(jnp.broadcast_to(array[None], (size, *array.shape)), axis, groups)


def summed(parts):
    return jnp.sum(parts.astype(f32), axis=0)


def dot_t(left, right, contract):
    return lax.dot_general(left, right, (contract, ((), ())), preferred_element_type=f32)


def pick(stack, index):
    return lax.dynamic_index_in_dim(stack, index, 0, keepdims=False)


def exchanged(stack, place, groups):
    got = [pick(stack, place)]
    for k in range(1, NEAR):
        pairs = [(g[i], g[i ^ k]) for g in groups for i in range(NEAR)]
        got.append(lax.ppermute(pick(stack, place ^ k), "kv", pairs))
    got = jnp.stack(got)
    return jnp.stack([pick(got, j ^ place) for j in range(NEAR)])


def step(
    tokens,
    mix_gain,
    w_query,
    w_forget,
    w_input,
    w_outgate,
    lower_bound,
    state,
    head_gain,
    w_mixout,
    ffn_gain,
    w_gate,
    w_up,
    w_down,
):
    rows_here, heads_here, head_size = state.shape[:3]
    kv, tp = lax.axis_size("kv"), lax.axis_size("tp")
    batch, own_width = tokens.shape
    far = kv // NEAR
    near_groups = [[NEAR * a + b for b in range(NEAR)] for a in range(far)]
    far_groups = [[NEAR * a + b for a in range(far)] for b in range(NEAR)]
    block_groups = [
        [(NEAR * a + b) * tp + t for b in range(NEAR) for t in range(tp)] for a in range(far)
    ]
    place = lax.axis_index("kv") % NEAR

    units = w_gate.shape[1] // NEAR
    width = -(-(2 * units + 1) // 128) * 128
    pad = jnp.zeros((w_gate.shape[0], width - 2 * units - 1), bf16)
    cut = lambda w, j: w[:, j * units : (j + 1) * units]
    rows = w_gate.shape[0]
    pieces = []
    for j in range(NEAR):
        both = jnp.concatenate([cut(w_gate, j), cut(w_up, j), ffn_gain[:, None], pad], axis=1)
        blocks = [both[:, at : at + 128] for at in range(0, width, 128)]
        pieces.append(jnp.concatenate(blocks + [w_down[j * units : (j + 1) * units]], axis=0))
    got = exchanged(jnp.stack(pieces), place, near_groups)
    at_down = width // 128 * rows
    w_out = got[:, at_down:]
    w_gate_up = jnp.concatenate(
        [got[:, at : at + rows].reshape(-1, 128) for at in range(0, at_down, rows)], axis=1
    )

    block = share(tokens.T, "tp", tp).reshape(-1, batch)
    block_f = block.astype(f32)
    normed = (block_f * mix_gain.astype(f32)[:, None]).astype(bf16)
    squares = jnp.sum(block_f * block_f, axis=0)
    weights = jnp.concatenate([w_query, w_forget, w_input, w_outgate], axis=1)
    terms = dot_t(normed, lax.optimization_barrier(weights), ((0,), (0,))).astype(bf16)
    side = jnp.broadcast_to(squares.astype(bf16)[:, None], (batch, 128))
    terms = jnp.concatenate([terms, side], axis=1)
    terms = terms.reshape(far, NEAR, rows_here, -1).transpose(1, 0, 2, 3)
    terms = summed(spread(terms, "kv", near_groups)).astype(bf16)
    sums = spread(terms, "kv", far_groups)
    sums = summed(sums)
    key_width = heads_here * head_size
    inv_rms = lax.rsqrt(sums[:, 4 * key_width : 4 * key_width + 1] / D + eps)
    raw = [
        (sums[:, i * key_width : (i + 1) * key_width] * inv_rms).reshape(
            rows_here, heads_here, head_size
        )
        for i in range(4)
    ]

    query_act = jax.nn.silu(raw[0])
    bounds = lower_bound.reshape(heads_here, head_size)
    forget = bounds + (1.0 - bounds) * jax.nn.sigmoid(raw[1])
    key_in = (1.0 - bounds) * jax.nn.sigmoid(-raw[1])
    new_state = forget[..., None] * state + key_in[..., None] * raw[2][:, :, None, :]
    readout = jnp.sum(query_act[..., None] * new_state, axis=2)
    head_rms = lax.rsqrt(jnp.mean(readout * readout, axis=-1, keepdims=True) + eps)
    gated = readout * head_rms * head_gain.astype(f32) * jax.nn.silu(raw[3])
    gated = gated.reshape(rows_here, key_width).astype(bf16)

    gated_all = share(gated, "kv", kv).reshape(batch, key_width)
    mix = dot_t(w_mixout, gated_all, ((0,), (1,))).astype(bf16)
    resid = (block_f + summed(share(mix, "tp", tp))).astype(bf16)
    resid_own = lax.dynamic_slice_in_dim(resid, lax.axis_index("tp") * own_width, own_width, 0)

    resid_f = share(resid, "kv", NEAR, near_groups).reshape(-1, batch).astype(f32)
    gain = w_gate_up[:, 2 * units : 2 * units + 1].astype(f32)
    normed_ffn = (resid_f * gain).astype(bf16)
    squares_ffn = jnp.sum(resid_f * resid_f, axis=0)
    terms = dot_t(normed_ffn, w_gate_up, ((0,), (0,)))
    column = lax.broadcasted_iota(jnp.int32, terms.shape, 1)
    terms = jnp.where(column == 2 * units, squares_ffn[:, None], terms).astype(bf16)
    sums = summed(spread(terms.reshape(far, -1, width), "kv", far_groups))
    inv_rms = lax.rsqrt(sums[:, 2 * units : 2 * units + 1] / D + eps)
    gate_sum, up_sum = sums[:, :units] * inv_rms, sums[:, units : 2 * units] * inv_rms
    hidden = (jax.nn.silu(gate_sum) * up_sum).astype(bf16)
    hidden_all = share(hidden, "kv", far, far_groups).reshape(batch, units)
    down = dot_t(w_out, hidden_all, ((1,), (1,))).astype(bf16)
    down = summed(spread(down.reshape(NEAR * tp, own_width, batch), ("kv", "tp"), block_groups))
    mixed = (resid_own.astype(f32) + down).astype(bf16).T
    return (mixed, new_state)


def solution(mesh):
    return jax.shard_map(
        step,
        mesh=mesh,
        in_specs=(
            P("grp", ("kv", "tp")),
            P("kv"),
            P("kv", "tp"),
            P("kv", "tp"),
            P("kv", "tp"),
            P("kv", "tp"),
            P("tp"),
            P(("grp", "kv"), "tp", None, None),
            P(),
            P("tp", "kv"),
            P("kv"),
            P("kv", "tp"),
            P("kv", "tp"),
            P("tp", "kv"),
        ),
        out_specs=(P("grp", ("kv", "tp")), P(("grp", "kv"), "tp", None, None)),
        check_vma=False,
    )
```

```python
import jax
import jax.numpy as jnp
from jax import lax
from jax.sharding import PartitionSpec as P


D = 4096
NEAR = 4

eps = 0.1
bf16, f32 = jnp.bfloat16, jnp.float32


def spread(parts, axis, groups=None):
    return lax.all_to_all(parts, axis, 0, 0, axis_index_groups=groups, tiled=True)


def share(array, axis, size, groups=None):
    return spread(jnp.broadcast_to(array[None], (size, *array.shape)), axis, groups)


def summed(parts):
    return jnp.sum(parts.astype(f32), axis=0)


def dot_t(left, right, contract):
    return lax.dot_general(left, right, (contract, ((), ())), preferred_element_type=f32)


def pick(stack, index):
    return lax.dynamic_index_in_dim(stack, index, 0, keepdims=False)


together = lax.optimization_barrier


def exchanged(stack, place, groups):
    got = [pick(stack, place)]
    for k in range(1, NEAR):
        pairs = [(g[i], g[i ^ k]) for g in groups for i in range(NEAR)]
        got.append(lax.ppermute(pick(stack, place ^ k), "kv", pairs))
    return got


def step(
    tokens,
    mix_gain,
    w_query,
    w_forget,
    w_input,
    w_outgate,
    lower_bound,
    state,
    head_gain,
    w_mixout,
    ffn_gain,
    w_gate,
    w_up,
    w_down,
):
    rows_here, heads_here, head_size = state.shape[:3]
    kv, tp = lax.axis_size("kv"), lax.axis_size("tp")
    batch, own_width = tokens.shape
    far = kv // NEAR
    near_groups = [[NEAR * a + b for b in range(NEAR)] for a in range(far)]
    far_groups = [[NEAR * a + b for a in range(far)] for b in range(NEAR)]
    block_groups = [
        [(NEAR * a + b) * tp + t for b in range(NEAR) for t in range(tp)] for a in range(far)
    ]
    place = lax.axis_index("kv") % NEAR

    units = w_gate.shape[1] // NEAR
    width = -(-(2 * units + 1) // 128) * 128
    pad = jnp.zeros((w_gate.shape[0], width - 2 * units - 1), bf16)
    cut = lambda w, j: w[:, j * units : (j + 1) * units]
    rows = w_gate.shape[0]
    pieces = []
    for j in range(NEAR):
        both = jnp.concatenate([cut(w_gate, j), cut(w_up, j), ffn_gain[:, None], pad], axis=1)
        blocks = [both[:, at : at + 128] for at in range(0, width, 128)]
        pieces.append(jnp.concatenate(blocks + [w_down[j * units : (j + 1) * units]], axis=0))
    pieces = jnp.stack(pieces)

    block = share(tokens.T, "tp", tp).reshape(-1, batch)
    weights = jnp.concatenate([w_query, w_forget, w_input, w_outgate], axis=1)
    own_at = (lax.axis_index("tp") * own_width).astype(jnp.uint32)
    is_square = lax.iota(jnp.int32, width) == 2 * units
    block, pieces, weights, lower_bound, head_gain, own_at, is_square = together(
        (block, pieces, weights, lower_bound, head_gain.astype(f32), own_at, is_square)
    )
    block_f = block.astype(f32)
    normed = (block_f * mix_gain.astype(f32)[:, None]).astype(bf16)
    squares = jnp.sum(block_f * block_f, axis=0)
    terms = dot_t(normed, weights, ((0,), (0,))).astype(bf16)
    side = jnp.broadcast_to(squares.astype(bf16)[:, None], (batch, 128))
    terms = jnp.concatenate([terms, side], axis=1)
    terms = terms.reshape(far, NEAR, rows_here, -1).transpose(1, 0, 2, 3)
    terms = summed(spread(terms, "kv", near_groups)).astype(bf16)
    terms, place = together((terms, place))
    got = exchanged(pieces, place, near_groups)
    sums = spread(terms, "kv", far_groups)
    sums = summed(sums)
    key_width = heads_here * head_size
    inv_rms = lax.rsqrt(sums[:, 4 * key_width : 4 * key_width + 1] / D + eps)
    raw = [
        (sums[:, i * key_width : (i + 1) * key_width] * inv_rms).reshape(
            rows_here, heads_here, head_size
        )
        for i in range(4)
    ]

    query_act = jax.nn.silu(raw[0])
    bounds = lower_bound.reshape(heads_here, head_size)
    forget = bounds + (1.0 - bounds) * jax.nn.sigmoid(raw[1])
    key_in = (1.0 - bounds) * jax.nn.sigmoid(-raw[1])
    new_state = forget[..., None] * state + key_in[..., None] * raw[2][:, :, None, :]
    readout = jnp.sum(query_act[..., None] * new_state, axis=2)
    head_rms = lax.rsqrt(jnp.mean(readout * readout, axis=-1, keepdims=True) + eps)
    gated = readout * head_rms * head_gain * jax.nn.silu(raw[3])
    gated = gated.reshape(rows_here, key_width).astype(bf16)

    gated, got[0] = together((gated, got[0]))
    got = jnp.stack(got)
    got = jnp.stack([pick(got, j ^ place) for j in range(NEAR)])
    at_down = width // 128 * rows
    w_out = got[:, at_down:]
    w_gate_up = jnp.concatenate(
        [got[:, at : at + rows].reshape(-1, 128) for at in range(0, at_down, rows)], axis=1
    )
    gain = w_gate_up[:, 2 * units : 2 * units + 1].astype(f32)

    gated_all = share(gated, "kv", kv).reshape(batch, key_width)
    mix = dot_t(w_mixout, gated_all, ((0,), (1,))).astype(bf16)
    mix, w_gate_up, w_out, gain = together((mix, w_gate_up, w_out, gain))
    resid = (block_f + summed(share(mix, "tp", tp))).astype(bf16)
    resid_own = lax.dynamic_slice(resid, (own_at, jnp.uint32(0)), (own_width, batch))
    resid, resid_own = together((resid, resid_own))

    resid_f = share(resid, "kv", NEAR, near_groups).reshape(-1, batch).astype(f32)
    normed_ffn = (resid_f * gain).astype(bf16)
    squares_ffn = jnp.sum(resid_f * resid_f, axis=0)
    terms = dot_t(normed_ffn, w_gate_up, ((0,), (0,)))
    terms = jnp.where(is_square, squares_ffn[:, None], terms).astype(bf16)
    sums = summed(spread(terms.reshape(far, -1, width), "kv", far_groups))
    inv_rms = lax.rsqrt(sums[:, 2 * units : 2 * units + 1] / D + eps)
    gate_sum, up_sum = sums[:, :units] * inv_rms, sums[:, units : 2 * units] * inv_rms
    hidden = (jax.nn.silu(gate_sum) * up_sum).astype(bf16)
    hidden_all = share(hidden, "kv", far, far_groups).reshape(batch, units)
    down = dot_t(w_out, hidden_all, ((1,), (1,))).astype(bf16)
    down = summed(spread(down.reshape(NEAR * tp, own_width, batch), ("kv", "tp"), block_groups))
    mixed = (resid_own.astype(f32) + down).astype(bf16).T
    return (mixed, new_state)


def solution(mesh):
    return jax.shard_map(
        step,
        mesh=mesh,
        in_specs=(
            P("grp", ("kv", "tp")),
            P("kv"),
            P("kv", "tp"),
            P("kv", "tp"),
            P("kv", "tp"),
            P("kv", "tp"),
            P("tp"),
            P(("grp", "kv"), "tp", None, None),
            P(),
            P("tp", "kv"),
            P("kv"),
            P("kv", "tp"),
            P("kv", "tp"),
            P("tp", "kv"),
        ),
        out_specs=(P("grp", ("kv", "tp")), P(("grp", "kv"), "tp", None, None)),
        check_vma=False,
    )
```

```python
import jax
import jax.numpy as jnp
from jax import lax
from jax.sharding import PartitionSpec as P


D = 4096
NEAR = 4

eps = 0.1
bf16, f32 = jnp.bfloat16, jnp.float32


def spread(parts, axis, groups=None):
    return lax.all_to_all(parts, axis, 0, 0, axis_index_groups=groups, tiled=True)


def share(array, axis, size, groups=None):
    return spread(jnp.broadcast_to(array[None], (size, *array.shape)), axis, groups)


def summed(parts):
    return jnp.sum(parts.astype(f32), axis=0)


def dot_t(left, right, contract):
    return lax.dot_general(left, right, (contract, ((), ())), preferred_element_type=f32)


def pick(stack, index):
    return lax.dynamic_index_in_dim(stack, index, 0, keepdims=False)


together = lax.optimization_barrier


def exchanged(stack, place, groups):
    got = [pick(stack, place)]
    for k in range(1, NEAR):
        pairs = [(g[i], g[i ^ k]) for g in groups for i in range(NEAR)]
        got.append(lax.ppermute(pick(stack, place ^ k), "kv", pairs))
    return got


def step(
    tokens,
    mix_gain,
    w_query,
    w_forget,
    w_input,
    w_outgate,
    lower_bound,
    state,
    head_gain,
    w_mixout,
    ffn_gain,
    w_gate,
    w_up,
    w_down,
):
    rows_here, heads_here, head_size = state.shape[:3]
    kv, tp = lax.axis_size("kv"), lax.axis_size("tp")
    batch, own_width = tokens.shape
    far = kv // NEAR
    near_groups = [[NEAR * a + b for b in range(NEAR)] for a in range(far)]
    far_groups = [[NEAR * a + b for a in range(far)] for b in range(NEAR)]
    block_groups = [
        [(NEAR * a + b) * tp + t for b in range(NEAR) for t in range(tp)] for a in range(far)
    ]
    place = lax.axis_index("kv") % NEAR

    units = w_gate.shape[1] // NEAR
    width = -(-(2 * units + 1) // 128) * 128
    rows = w_gate.shape[0]

    block = share(tokens.T, "tp", tp).reshape(-1, batch)
    weights = jnp.concatenate([w_query, w_forget, w_input, w_outgate], axis=1)
    own_at = (lax.axis_index("tp") * own_width).astype(jnp.uint32)
    is_square = lax.iota(jnp.int32, width) == 2 * units
    block, weights, lower_bound, head_gain, own_at, is_square = together(
        (block, weights, lower_bound, head_gain.astype(f32), own_at, is_square)
    )
    block_f = block.astype(f32)
    normed = (block_f * mix_gain.astype(f32)[:, None]).astype(bf16)
    squares = jnp.sum(block_f * block_f, axis=0)
    terms = dot_t(normed, weights, ((0,), (0,))).astype(bf16)
    side = jnp.broadcast_to(squares.astype(bf16)[:, None], (batch, 128))
    terms = jnp.concatenate([terms, side], axis=1)
    terms = terms.reshape(far, NEAR, rows_here, -1).transpose(1, 0, 2, 3)
    terms = spread(terms, "kv", near_groups)

    pad = jnp.zeros((rows, width - 2 * units - 1), bf16)
    cut = lambda w, j: w[:, j * units : (j + 1) * units]
    pieces = []
    for j in range(NEAR):
        both = jnp.concatenate([cut(w_gate, j), cut(w_up, j), ffn_gain[:, None], pad], axis=1)
        blocks = [both[:, at : at + 128] for at in range(0, width, 128)]
        pieces.append(jnp.concatenate(blocks + [w_down[j * units : (j + 1) * units]], axis=0))
    pieces = jnp.stack(pieces)

    terms, pieces, place = together((terms, pieces, place))
    terms = summed(terms).astype(bf16)
    got = exchanged(pieces, place, near_groups)
    sums = spread(terms, "kv", far_groups)
    sums = summed(sums)
    key_width = heads_here * head_size
    inv_rms = lax.rsqrt(sums[:, 4 * key_width : 4 * key_width + 1] / D + eps)
    raw = [
        (sums[:, i * key_width : (i + 1) * key_width] * inv_rms).reshape(
            rows_here, heads_here, head_size
        )
        for i in range(4)
    ]

    query_act = jax.nn.silu(raw[0])
    bounds = lower_bound.reshape(heads_here, head_size)
    forget = bounds + (1.0 - bounds) * jax.nn.sigmoid(raw[1])
    key_in = (1.0 - bounds) * jax.nn.sigmoid(-raw[1])
    from_state = jnp.sum((query_act * forget)[..., None] * state, axis=2)
    readout = from_state + jnp.sum(query_act * key_in, axis=-1, keepdims=True) * raw[2]
    head_rms = lax.rsqrt(jnp.mean(readout * readout, axis=-1, keepdims=True) + eps)
    gated = readout * head_rms * head_gain * jax.nn.silu(raw[3])
    gated = gated.reshape(rows_here, key_width).astype(bf16)

    gated, got[0], forget, key_in, values_in = together((gated, got[0], forget, key_in, raw[2]))
    new_state = forget[..., None] * state + key_in[..., None] * values_in[:, :, None, :]
    got = jnp.stack(got)
    got = jnp.stack([pick(got, j ^ place) for j in range(NEAR)])
    at_down = width // 128 * rows
    w_out = got[:, at_down:]
    w_gate_up = jnp.concatenate(
        [got[:, at : at + rows].reshape(-1, 128) for at in range(0, at_down, rows)], axis=1
    )
    gain = w_gate_up[:, 2 * units : 2 * units + 1].astype(f32)

    gated_all = share(gated, "kv", kv).reshape(batch, key_width)
    mix = dot_t(w_mixout, gated_all, ((0,), (1,))).astype(bf16)
    mix, w_gate_up, w_out, gain, new_state = together((mix, w_gate_up, w_out, gain, new_state))
    resid = (block_f + summed(share(mix, "tp", tp))).astype(bf16)
    resid_own = lax.dynamic_slice(resid, (own_at, jnp.uint32(0)), (own_width, batch))
    resid, resid_own = together((resid, resid_own))

    resid_f = share(resid, "kv", NEAR, near_groups).reshape(-1, batch).astype(f32)
    normed_ffn = (resid_f * gain).astype(bf16)
    squares_ffn = jnp.sum(resid_f * resid_f, axis=0)
    terms = dot_t(normed_ffn, w_gate_up, ((0,), (0,)))
    terms = jnp.where(is_square, squares_ffn[:, None], terms).astype(bf16)
    sums = summed(spread(terms.reshape(far, -1, width), "kv", far_groups))
    inv_rms = lax.rsqrt(sums[:, 2 * units : 2 * units + 1] / D + eps)
    gate_sum, up_sum = sums[:, :units] * inv_rms, sums[:, units : 2 * units] * inv_rms
    hidden = (jax.nn.silu(gate_sum) * up_sum).astype(bf16)
    hidden_all = share(hidden, "kv", far, far_groups).reshape(batch, units)
    down = dot_t(w_out, hidden_all, ((1,), (1,))).astype(bf16)
    down = summed(spread(down.reshape(NEAR * tp, own_width, batch), ("kv", "tp"), block_groups))
    mixed = (resid_own.astype(f32) + down).astype(bf16).T
    return (mixed, new_state)


def solution(mesh):
    return jax.shard_map(
        step,
        mesh=mesh,
        in_specs=(
            P("grp", ("kv", "tp")),
            P("kv"),
            P("kv", "tp"),
            P("kv", "tp"),
            P("kv", "tp"),
            P("kv", "tp"),
            P("tp"),
            P(("grp", "kv"), "tp", None, None),
            P(),
            P("tp", "kv"),
            P("kv"),
            P("kv", "tp"),
            P("kv", "tp"),
            P("tp", "kv"),
        ),
        out_specs=(P("grp", ("kv", "tp")), P(("grp", "kv"), "tp", None, None)),
        check_vma=False,
    )
```

```python
import jax
import jax.numpy as jnp
from jax import lax
from jax.sharding import PartitionSpec as P


D = 4096
NEAR = 4

eps = 0.1
bf16, f32 = jnp.bfloat16, jnp.float32


def spread(parts, axis, groups=None):
    return lax.all_to_all(parts, axis, 0, 0, axis_index_groups=groups, tiled=True)


def share(array, axis, size, groups=None):
    return spread(jnp.broadcast_to(array[None], (size, *array.shape)), axis, groups)


def summed(parts):
    return jnp.sum(parts.astype(f32), axis=0)


def dot_t(left, right, contract):
    return lax.dot_general(left, right, (contract, ((), ())), preferred_element_type=f32)


def pick(stack, index):
    return lax.dynamic_index_in_dim(stack, index, 0, keepdims=False)


together = lax.optimization_barrier


def exchanged(stack, place, groups):
    got = [pick(stack, place)]
    for k in range(1, NEAR):
        pairs = [(g[i], g[i ^ k]) for g in groups for i in range(NEAR)]
        got.append(lax.ppermute(pick(stack, place ^ k), "kv", pairs))
    return got


def step(
    tokens,
    mix_gain,
    w_query,
    w_forget,
    w_input,
    w_outgate,
    lower_bound,
    state,
    head_gain,
    w_mixout,
    ffn_gain,
    w_gate,
    w_up,
    w_down,
):
    rows_here, heads_here, head_size = state.shape[:3]
    kv, tp = lax.axis_size("kv"), lax.axis_size("tp")
    batch, own_width = tokens.shape
    far = kv // NEAR
    near_groups = [[NEAR * a + b for b in range(NEAR)] for a in range(far)]
    far_groups = [[NEAR * a + b for a in range(far)] for b in range(NEAR)]
    block_groups = [
        [(NEAR * a + b) * tp + t for b in range(NEAR) for t in range(tp)] for a in range(far)
    ]
    place = lax.axis_index("kv") % NEAR

    units = w_gate.shape[1] // NEAR
    width = -(-(2 * units + 1) // 128) * 128
    rows = w_gate.shape[0]

    block = share(tokens.T, "tp", tp).reshape(-1, batch)
    weights = jnp.concatenate([w_query, w_forget, w_input, w_outgate], axis=1)
    own_at = (lax.axis_index("tp") * own_width).astype(jnp.uint32)
    is_square = lax.iota(jnp.int32, width) == 2 * units
    block, weights, lower_bound, head_gain, own_at, is_square = together(
        (block, weights, lower_bound, head_gain.astype(f32), own_at, is_square)
    )
    block_f = block.astype(f32)
    normed = (block_f * mix_gain.astype(f32)[:, None]).astype(bf16)
    squares = jnp.sum(block_f * block_f, axis=0)
    terms = dot_t(normed, weights, ((0,), (0,))).astype(bf16)
    side = jnp.broadcast_to(squares.astype(bf16)[:, None], (batch, 128))
    terms = jnp.concatenate([terms, side], axis=1)
    terms = terms.reshape(far, NEAR, rows_here, -1).transpose(1, 0, 2, 3)
    terms = spread(terms, "kv", near_groups)

    cut = lambda w, j: w[:, j * units : (j + 1) * units]
    whole = 2 * units // rows * rows
    rest = 2 * units - whole
    folds = rows // rest
    gains = jnp.broadcast_to(ffn_gain[None], (16, rows))
    pieces = []
    for j in range(NEAR):
        both = jnp.concatenate([cut(w_gate, j), cut(w_up, j)], axis=1)
        blocks = [both[:, at : at + rows] for at in range(0, whole, rows)]
        folded = both[:, whole:].reshape(folds, rest, rest)
        blocks.append(jnp.concatenate([folded[i] for i in range(folds)], axis=1))
        blocks += [w_down[j * units : (j + 1) * units], gains]
        pieces.append(jnp.concatenate(blocks, axis=0))
    pieces = jnp.stack(pieces)

    terms, pieces, place = together((terms, pieces, place))
    terms = summed(terms).astype(bf16)
    got = exchanged(pieces, place, near_groups)
    sums = spread(terms, "kv", far_groups)
    sums = summed(sums)
    key_width = heads_here * head_size
    inv_rms = lax.rsqrt(sums[:, 4 * key_width : 4 * key_width + 1] / D + eps)
    raw = [
        (sums[:, i * key_width : (i + 1) * key_width] * inv_rms).reshape(
            rows_here, heads_here, head_size
        )
        for i in range(4)
    ]

    query_act = jax.nn.silu(raw[0])
    bounds = lower_bound.reshape(heads_here, head_size)
    forget = bounds + (1.0 - bounds) * jax.nn.sigmoid(raw[1])
    key_in = (1.0 - bounds) * jax.nn.sigmoid(-raw[1])
    from_state = jnp.sum((query_act * forget)[..., None] * state, axis=2)
    readout = from_state + jnp.sum(query_act * key_in, axis=-1, keepdims=True) * raw[2]
    head_rms = lax.rsqrt(jnp.mean(readout * readout, axis=-1, keepdims=True) + eps)
    gated = readout * head_rms * head_gain * jax.nn.silu(raw[3])
    gated = gated.reshape(rows_here, key_width).astype(bf16)

    gated, got[0], forget, key_in, values_in = together((gated, got[0], forget, key_in, raw[2]))
    new_state = forget[..., None] * state + key_in[..., None] * values_in[:, :, None, :]
    got = jnp.stack(got)
    got = jnp.stack([pick(got, j ^ place) for j in range(NEAR)])
    folded = got[:, whole : whole + rest]
    folded = [folded[..., i * rest : (i + 1) * rest] for i in range(folds)]
    blocks = [got[:, at : at + rows].reshape(-1, rows) for at in range(0, whole, rows)]
    blocks.append(jnp.concatenate(folded, axis=1).reshape(-1, rest))
    blocks.append(jnp.zeros((NEAR * rows, width - 2 * units), bf16))
    w_gate_up = jnp.concatenate(blocks, axis=1)
    w_out = got[:, whole + rest : whole + rest + units]
    gain = got[:, whole + rest + units].reshape(-1, 1).astype(f32)

    gated_all = share(gated, "kv", kv).reshape(batch, key_width)
    mix = dot_t(w_mixout, gated_all, ((0,), (1,))).astype(bf16)
    mix, w_gate_up, w_out, gain, new_state = together((mix, w_gate_up, w_out, gain, new_state))
    resid = (block_f + summed(share(mix, "tp", tp))).astype(bf16)
    resid_own = lax.dynamic_slice(resid, (own_at, jnp.uint32(0)), (own_width, batch))
    resid, resid_own = together((resid, resid_own))

    resid_f = share(resid, "kv", NEAR, near_groups).reshape(-1, batch).astype(f32)
    normed_ffn = (resid_f * gain).astype(bf16)
    squares_ffn = jnp.sum(resid_f * resid_f, axis=0)
    terms = dot_t(normed_ffn, w_gate_up, ((0,), (0,)))
    terms = jnp.where(is_square, squares_ffn[:, None], terms).astype(bf16)
    sums = summed(spread(terms.reshape(far, -1, width), "kv", far_groups))
    inv_rms = lax.rsqrt(sums[:, 2 * units : 2 * units + 1] / D + eps)
    gate_sum, up_sum = sums[:, :units] * inv_rms, sums[:, units : 2 * units] * inv_rms
    hidden = (jax.nn.silu(gate_sum) * up_sum).astype(bf16)
    hidden_all = share(hidden, "kv", far, far_groups).reshape(batch, units)
    down = dot_t(w_out, hidden_all, ((1,), (1,))).astype(bf16)
    down = summed(spread(down.reshape(NEAR * tp, own_width, batch), ("kv", "tp"), block_groups))
    mixed = (resid_own.astype(f32) + down).astype(bf16).T
    return (mixed, new_state)


def solution(mesh):
    return jax.shard_map(
        step,
        mesh=mesh,
        in_specs=(
            P("grp", ("kv", "tp")),
            P("kv"),
            P("kv", "tp"),
            P("kv", "tp"),
            P("kv", "tp"),
            P("kv", "tp"),
            P("tp"),
            P(("grp", "kv"), "tp", None, None),
            P(),
            P("tp", "kv"),
            P("kv"),
            P("kv", "tp"),
            P("kv", "tp"),
            P("tp", "kv"),
        ),
        out_specs=(P("grp", ("kv", "tp")), P(("grp", "kv"), "tp", None, None)),
        check_vma=False,
    )
```
